256 devices in a mesh: ep: 128 (over z, y, x), tp: 2 (over core).
Axes of the slice: x: 4, y: 4, z: 8, core: 2. Of those that a mesh axis runs over, the one named last changes fastest.
Arguments:
- tokens: bfloat16 [65536, 2048], P(('ep', 'tp')), may hold values from -6 to 6
- norm_gain: float32 [2048], replicated, may hold values from 0.1 to 1.9
- expert_ids: int32 [65536, 2], P(('ep', 'tp')), may hold values from 0 to 127, all different within a row; in each aligned block of 256 rows (0 to 255, 256 to 511, ...) at most 6 rows name the same one
- route_weights: float32 [65536, 2], P(('ep', 'tp')), may hold values from 0.2 to 1.2
- expert_gate: bfloat16 [128, 2048, 512], P('ep', None, 'tp'), may hold values from -0.125 to 0.125
- expert_up: bfloat16 [128, 2048, 512], P('ep', None, 'tp'), may hold values from -0.125 to 0.125
- expert_down: bfloat16 [128, 512, 2048], P('ep', 'tp'), may hold values from -0.25 to 0.25
- shared_gate: bfloat16 [2048, 512], P(None, 'tp'), may hold values from -0.125 to 0.125
- shared_up: bfloat16 [2048, 512], P(None, 'tp'), may hold values from -0.125 to 0.125
- shared_down: bfloat16 [512, 2048], P('tp'), may hold values from -0.25 to 0.25
Outputs:
- mixed: bfloat16 [65536, 2048], P(('ep', 'tp'))
The draws below stay inside these ranges and needn't reach their ends.
Inputs may be any that keep to these rules, and one draw needn't show every extreme that they name: `expert_ids`: each token names 2 different experts. Among the tokens of one device (aligned blocks of 256 rows) no expert is named by more than 6 tokens, and in every block some expert is named by exactly 6.
All inputs are finite; a program needn't handle non-finite values.
Results may differ from the reference program's by a relative error of at most 0.0075.
Values may be sent and summed in bfloat16 or wider, within the bound.
A program may use at most 64 MiB of HBM per device.

```python
import math
import jax
import jax.numpy as jnp
import numpy as np
from jax import lax

D = 2048
DE = 512
DS = 512
TOP_K = 2
TOK_DEV = 256
EXPERTS = 128
CAP = 6
TOKENS = 65536
N_EP = 128
N_TP = 2


def block_scale(key, shape, pieces, smallest, top_value):
    factor_of, own = 1.0, jax.random.fold_in(key, 6)
    for axis_at, blocks in pieces:
        draws = jnp.exp(jax.random.uniform(jax.random.fold_in(own, axis_at), (blocks,), jnp.float32, smallest / len(pieces), top_value / len(pieces)))
        factor_of = factor_of * jnp.repeat(draws, shape[axis_at] // blocks).reshape([-1 if axis == axis_at else 1 for axis in range(len(shape))])
    return factor_of


def assign_block(key, own, number, rows, amount, top, most, skew):
    order = jax.random.permutation(key, amount)
    heavy_load, ordinary = load_shares(amount, rows * top, most, skew, True), load_shares(amount, rows * top, most, skew, False)
    places = jnp.arange(amount)

    def named(lengths, offset_by):
        used = int((lengths > 0).sum())
        fixed = max(1, used // 4)
        moved = fixed + (places - fixed + offset_by * (used - fixed)) % max(1, amount - fixed)
        return jnp.zeros((amount,), jnp.int32).at[order[jnp.where(places < fixed, places, moved)]].set(jnp.asarray(lengths, jnp.int32))

    lengths = jnp.where(number % 4 == 0, named(heavy_load, number // 4), named(ordinary, number - number // 4 - 1))
    mixed = jax.random.permutation(jax.random.fold_in(own, 3), amount)
    giver, sink = mixed[0:amount // 2 * 2:2], mixed[1:amount // 2 * 2:2]
    slack = jnp.minimum(lengths[giver] - 1, most - lengths[sink]) // 2
    slack = jnp.where((giver == order[0]) | (sink == order[0]) | (lengths[sink] == 0), 0, jnp.maximum(slack, 0))
    moved = jax.random.randint(jax.random.fold_in(own, 4), (amount // 2,), 0, 1 << 20) % (slack + 1)
    lengths = lengths.at[giver].add(-moved).at[sink].add(moved)
    items = jnp.searchsorted(jnp.cumsum(lengths), jnp.arange(rows * top), side="right").astype(jnp.int32)
    grid = items.reshape(top, rows).T
    grid = grid[jax.random.permutation(jax.random.fold_in(own, 1), rows)]
    offset_by = jax.random.randint(jax.random.fold_in(own, 2), (rows, 1), 0, top)
    return jnp.take_along_axis(grid, (jnp.arange(top)[None, :] + offset_by) % top, axis=1)


def load_shares(number_of, total, limit, skew, full):
    portions = [(1 << 20) // math.isqrt(standing ** skew) + 1 for standing in range(1, number_of + 1)]
    largest = limit if full else min(limit, max(-(-total // number_of), total * portions[0] // sum(portions)))
    least = 1 if total - largest >= number_of - 1 else 0
    holding, spare = [largest] + [least] * (number_of - 1), total - largest - least * (number_of - 1)
    while spare > 0:
        movable = [i for i in range(1, number_of) if holding[i] < largest] or [i for i in range(1, number_of) if holding[i] < limit]
        mass, left = sum([portions[i] for i in movable]), spare
        for i in movable:
            addition = min(limit - holding[i], max(1, left * portions[i] // mass), spare)
            holding[i] = holding[i] + addition
            spare = spare - addition
    return np.array(holding)


def noise(own_key, extent, spread, reach, split=(), kind=jnp.bfloat16):
    gain = block_scale(own_key, extent, split, -0.22, 0.18) if split else 1.0
    array = jax.random.normal(own_key, extent, jnp.float32) * spread * gain
    return jnp.minimum(jnp.maximum(array, -reach), reach).astype(kind)


def setup_inputs(seed: int = 0) -> dict:
    key_of = jax.random.split(jax.random.key(seed), 11)
    tokens = noise(key_of[0], (TOKENS, D), 1.0, 6.0, ((0, 256),))
    norm_gain = jnp.clip(1.0 + 0.18 * jax.random.normal(key_of[1], (D,), jnp.float32), 0.1, 1.9)
    expert_ids_keys = jax.random.split(jax.random.fold_in(key_of[2], 1), TOKENS // TOK_DEV)
    expert_ids_turns = jax.random.permutation(jax.random.fold_in(key_of[2], 3), TOKENS // TOK_DEV)
    expert_ids = jax.vmap(lambda own, number: assign_block(jax.random.fold_in(key_of[2], 2), own, number, TOK_DEV, EXPERTS, TOP_K, CAP, 2))(expert_ids_keys, expert_ids_turns).reshape((TOKENS, TOP_K))
    route_weights = jnp.clip(0.2 + 1 * jax.random.uniform(key_of[3], (TOKENS, TOP_K), jnp.float32) ** block_scale(key_of[3], (TOKENS, TOP_K), ((0, 256),), -0.2, 0.2), 0.2, 1.2)
    expert_gate = noise(key_of[4], (EXPERTS, D, DE), D ** -0.5, 0.125, ((0, 128), (2, 2)))
    expert_up = noise(key_of[5], (EXPERTS, D, DE), D ** -0.5, 0.125, ((0, 128), (2, 2)))
    expert_down = noise(key_of[6], (EXPERTS, DE, D), DE ** -0.5, 0.25, ((0, 128), (1, 2)))
    shared_gate = noise(key_of[7], (D, DS), D ** -0.5, 0.125, ((1, 2),))
    shared_up = noise(key_of[8], (D, DS), D ** -0.5, 0.125, ((1, 2),))
    shared_down = noise(key_of[9], (DS, D), DS ** -0.5, 0.25, ((0, 2),))
    return {"tokens": tokens, "norm_gain": norm_gain, "expert_ids": expert_ids, "route_weights": route_weights, "expert_gate": expert_gate, "expert_up": expert_up, "expert_down": expert_down, "shared_gate": shared_gate, "shared_up": shared_up, "shared_down": shared_down}


epsilon = 1e-06

def normalize(tokens, norm_gain):
    values = tokens.astype(jnp.float32)
    factor = lax.rsqrt(lax.optimization_barrier(jnp.mean(values * values, axis=1, keepdims=True)) + epsilon)
    return (values * factor * norm_gain[None, :]).astype(jnp.bfloat16)

def halves(row_block, gate_w, up_w, down_w):
    half_width = gate_w.shape[1] // N_TP
    summed = jnp.zeros((row_block.shape[0], down_w.shape[1]), jnp.float32)
    for portion in range(N_TP):
        first = portion * half_width
        gate_value = jnp.dot(row_block, gate_w[:, first:first + half_width], preferred_element_type=jnp.float32)
        up_value = jnp.dot(row_block, up_w[:, first:first + half_width], preferred_element_type=jnp.float32)
        hidden = (jax.nn.silu(gate_value) * up_value).astype(jnp.bfloat16)
        partial_value = jnp.dot(hidden, down_w[first:first + half_width], preferred_element_type=jnp.float32)
        rounded = lax.optimization_barrier(partial_value.astype(jnp.bfloat16))
        summed = summed + rounded.astype(jnp.float32)
    return summed

def reference(tokens, norm_gain, expert_ids, route_weights, expert_gate, expert_up, expert_down, shared_gate, shared_up, shared_down):
    normed = normalize(tokens, norm_gain)
    total_rows = tokens.shape[0]
    shared_out = halves(normed, shared_gate, shared_up, shared_down)
    flat_ids = expert_ids.reshape(-1).astype(jnp.int32)
    assigned = flat_ids.shape[0]
    ordering = jnp.argsort(flat_ids, stable=True).astype(jnp.int32)
    counts = jnp.bincount(flat_ids, length=EXPERTS).astype(jnp.int32)
    starts = (jnp.cumsum(counts) - counts).astype(jnp.int32)
    most_rows = N_EP * N_TP * CAP
    padded = jnp.concatenate([normed, jnp.zeros((1, D), jnp.bfloat16)], axis=0)
    flat_weights = route_weights.reshape(-1)

    def per_expert(totals, expert):
        slot_range = jnp.arange(most_rows, dtype=jnp.int32)
        filled = slot_range < counts[expert]
        row_index = jnp.minimum(starts[expert] + slot_range, assigned - 1)
        assign = jnp.where(filled, ordering[row_index], assigned)
        token_index = (assign // TOP_K).astype(jnp.int32)
        row_block = padded[token_index]
        expert_out = halves(row_block, expert_gate[expert], expert_up[expert], expert_down[expert]).astype(jnp.bfloat16)
        weight_rows = jnp.where(filled, flat_weights[jnp.minimum(assign, assigned - 1)], jnp.float32(0.0))
        totals = totals.at[token_index].add(expert_out.astype(jnp.float32) * weight_rows[:, None])
        return (totals, None)
    totals, _ = lax.scan(per_expert, jnp.zeros((total_rows + 1, D), jnp.float32), jnp.arange(EXPERTS, dtype=jnp.int32))
    routed = totals[:total_rows]
    return (routed + shared_out).astype(jnp.bfloat16)
```

```python
import functools

import jax
import jax.numpy as jnp
from jax import lax
from jax.experimental import pallas as pl
from jax.experimental.pallas import tpu as pltpu
from jax.sharding import PartitionSpec as P

MESH = pl.DeviceIdType.MESH
F32, BF16 = jnp.float32, jnp.bfloat16
epsilon = 1e-06
LANES, SUB = 128, 16
NZ, NY, NX = 8, 4, 4


def kernel(
    tokens_ref, gain_ref, ids_ref, weights_ref, eg_ref, eu_ref, ed_ref, sg_ref, su_ref, sd_ref,
    out_ref,
    normed, outgoing, received, results, returned, stage, rows, total, pcol, prow,
    wg, wu, wd, vg, vu, vd,
    local_sem, half_send, half_recv, out_send, out_recv, back_send, back_recv,
):
    plane = NY * NX
    experts = NZ * plane
    tok = tokens_ref.shape[0]
    capacity = received.shape[1] // SUB
    many = plane * capacity
    me, core = lax.axis_index("ep"), lax.axis_index("tp")
    z, y, x = me // plane, (me // NX) % NY, me % NX

    def at(dz, dy, dx):
        return ((z + dz) % NZ) * plane + ((y + dy) % NY) * NX + (x + dx) % NX

    barrier = pltpu.get_barrier_semaphore()

    def greet(step, carry):
        there = at(step // plane, (step // NX) % NY, step % NX)
        pl.semaphore_signal(barrier, inc=1, device_id=(there, core), device_id_type=MESH)
        return carry

    lax.fori_loop(1, experts, greet, 0)
    pl.semaphore_signal(barrier, inc=1, device_id=(me, 1 - core), device_id_type=MESH)

    pairs = (
        (sg_ref, vg), (su_ref, vu), (sd_ref, vd), (eg_ref.at[0], wg), (eu_ref.at[0], wu), (ed_ref.at[0], wd),
    )
    own = [pltpu.make_async_copy(a, b.at[0], local_sem.at[i]) for i, (a, b) in enumerate(pairs)]
    other = [
        pltpu.make_async_remote_copy(
            src_ref=a, dst_ref=b.at[1], send_sem=half_send.at[i], recv_sem=half_recv.at[i],
            device_id=(me, 1 - core), device_id_type=MESH,
        )
        for i, (a, b) in enumerate(pairs)
    ]
    for copy in own:
        copy.start()

    values = tokens_ref[...].astype(F32)
    factor = lax.rsqrt(jnp.mean(values * values, axis=1, keepdims=True) + epsilon)
    normed[...] = (values * factor * gain_ref[...]).astype(BF16)

    expert_at = lax.broadcasted_iota(jnp.int32, (tok, experts), 1)
    lower = (
        lax.broadcasted_iota(jnp.int32, (tok, tok), 0) > lax.broadcasted_iota(jnp.int32, (tok, tok), 1)
    ).astype(BF16)
    base = jnp.zeros((1, experts), F32)
    for j in range(2):
        named = ids_ref[:, j : j + 1]
        hot = (named == expert_at).astype(F32)
        before = jnp.dot(lower, hot.astype(BF16), preferred_element_type=F32) + base
        slot = jnp.sum(hot * before, axis=1, keepdims=True)
        base = base + jnp.sum(hot, axis=0, keepdims=True)
        position = jnp.broadcast_to(named.astype(F32) * capacity + slot, (tok, LANES))
        pcol[j] = position.astype(jnp.int32)
        prow[j] = jnp.transpose(position)[0:8].astype(jnp.int32)

    pl.semaphore_wait(barrier, experts)

    def turn(step):
        odd = step % 2
        return odd * ((step + 1) // 2) + (1 - odd) * ((NZ - step // 2) % NZ)

    def to_rows(source, first):
        flat = source[pl.ds(first, plane)].reshape(many * SUB, LANES)
        stage[...] = flat.astype(F32)
        for c in range(SUB):
            rows[:, c * LANES : (c + 1) * LANES] = stage[pl.ds(c, many, stride=SUB), :].astype(BF16)

    def from_block(block, c, width):
        for k in range(width // LANES):
            stage[pl.ds(c * (width // LANES) + k, many, stride=SUB), :] = block[:, k * LANES : (k + 1) * LANES]

    def to_flat(target, first):
        target[pl.ds(first, plane)] = stage[...].astype(BF16).reshape(plane, capacity * SUB, LANES)

    def dispatch(step, carry):
        dz = turn(step)
        zt = (z + dz) % NZ
        slots = lax.broadcasted_iota(jnp.int32, (many, tok), 0) + zt * many
        pick = ((slots == prow[0, 0:1]) | (slots == prow[1, 0:1])).astype(BF16)
        width = 256
        for c in range(SUB * LANES // width):
            from_block(
                jnp.dot(pick, normed[:, c * width : (c + 1) * width], preferred_element_type=F32), c, width
            )
        to_flat(outgoing, zt * plane)

        def send(i, carry):
            there = at(dz, i // NX, i % NX)
            pltpu.make_async_remote_copy(
                src_ref=outgoing.at[there], dst_ref=received.at[me], send_sem=out_send,
                recv_sem=out_recv.at[dz], device_id=(there, core), device_id_type=MESH,
            ).start()
            return carry

        @pl.when(step == 0)
        def _():
            pltpu.make_async_copy(outgoing.at[me], received.at[me], out_recv.at[0]).start()

        lax.fori_loop(jnp.where(step == 0, 1, 0), plane, send, 0)
        return carry

    lax.fori_loop(0, NZ, dispatch, 0)
    for copy in other:
        copy.start()

    def gated(block, gate_w, up_w):
        parts = []
        for h in range(2):
            gate = jnp.dot(block, gate_w[h], preferred_element_type=F32)
            up = jnp.dot(block, up_w[h], preferred_element_type=F32)
            parts.append((gate / (1.0 + jnp.exp(-gate)) * up).astype(BF16))
        return parts

    def down(parts, down_w, c, width):
        return sum(
            jnp.dot(parts[h], down_w[h, :, c * width : (c + 1) * width], preferred_element_type=F32)
            for h in range(2)
        )

    for i in range(3):
        own[i].wait()
        other[i].wait()
    step_rows = tok // 2

    def shared(step, carry):
        at_rows = pl.ds(pl.multiple_of(step * step_rows, step_rows), step_rows)
        parts = gated(normed[at_rows, :], vg, vu)
        for c in range(4):
            total[at_rows, c * 512 : (c + 1) * 512] = down(parts, vd, c, 512)
        return carry

    lax.fori_loop(0, 2, shared, 0)
    for i in range(3, 6):
        own[i].wait()
        other[i].wait()

    def expert(step, carry):
        dz = turn(step)
        zs = (z + NZ - dz) % NZ
        pltpu.make_async_remote_copy(
            src_ref=outgoing.at[pl.ds(0, plane)], dst_ref=received.at[pl.ds(zs * plane, plane)],
            send_sem=out_send, recv_sem=out_recv.at[dz], device_id=(me, 1 - core), device_id_type=MESH,
        ).wait_recv()
        to_rows(received, zs * plane)
        parts = gated(rows[...], wg, wu)
        for c in range(4):
            from_block(down(parts, wd, c, 512), c, 512)
        to_flat(results, zs * plane)

        def send(i, carry):
            there = at(NZ - dz, i // NX, i % NX)
            pltpu.make_async_remote_copy(
                src_ref=results.at[there], dst_ref=returned.at[me], send_sem=back_send,
                recv_sem=back_recv.at[dz], device_id=(there, core), device_id_type=MESH,
            ).start()
            return carry

        @pl.when(step == 0)
        def _():
            pltpu.make_async_copy(results.at[me], returned.at[me], back_recv.at[0]).start()

        lax.fori_loop(jnp.where(step == 0, 1, 0), plane, send, 0)
        return carry

    lax.fori_loop(0, NZ, expert, 0)

    def combine(step, carry):
        dz = turn(step)
        zt = (z + dz) % NZ
        pltpu.make_async_remote_copy(
            src_ref=results.at[pl.ds(0, plane)], dst_ref=returned.at[pl.ds(zt * plane, plane)],
            send_sem=back_send, recv_sem=back_recv.at[dz], device_id=(me, 1 - core), device_id_type=MESH,
        ).wait_recv()
        to_rows(returned, zt * plane)
        slots = lax.broadcasted_iota(jnp.int32, (tok, many), 1) + zt * many
        share = jnp.zeros((tok, many), F32)
        for j in range(2):
            share = share + jnp.where(slots == pcol[j, :, 0:1], weights_ref[:, j : j + 1], 0.0)
        high = share.astype(BF16)
        low = (share - high.astype(F32)).astype(BF16)
        for c in range(4):
            part = rows[:, c * 512 : (c + 1) * 512]
            total[:, c * 512 : (c + 1) * 512] += jnp.dot(
                high, part, preferred_element_type=F32
            ) + jnp.dot(low, part, preferred_element_type=F32)
        return carry

    lax.fori_loop(0, NZ, combine, 0)
    out_ref[...] = total[...].astype(BF16)

    pltpu.make_async_remote_copy(
        src_ref=outgoing.at[pl.ds(0, experts - 1)], dst_ref=received.at[pl.ds(0, experts - 1)],
        send_sem=out_send, recv_sem=out_recv.at[0], device_id=(me, 1 - core), device_id_type=MESH,
    ).wait_send()
    pltpu.make_async_remote_copy(
        src_ref=results.at[pl.ds(0, experts - 1)], dst_ref=returned.at[pl.ds(0, experts - 1)],
        send_sem=back_send, recv_sem=back_recv.at[0], device_id=(me, 1 - core), device_id_type=MESH,
    ).wait_send()


def body(tokens, norm_gain, expert_ids, route_weights, eg, eu, ed, sg, su, sd):
    tok, width = tokens.shape
    experts = eg.shape[0] * lax.axis_size("ep")
    capacity = 3 * tok * expert_ids.shape[1] // (2 * experts)
    many = NY * NX * capacity
    half, half_shared = eg.shape[2], sg.shape[1]
    slots = pltpu.VMEM((experts, capacity * SUB, LANES), BF16)
    vmem, hbm = pl.BlockSpec(memory_space=pltpu.VMEM), pl.BlockSpec(memory_space=pl.ANY)
    dma = pltpu.SemaphoreType.DMA
    return pl.pallas_call(
        kernel,
        out_shape=jax.ShapeDtypeStruct((tok, width), BF16),
        in_specs=[vmem] * 4 + [hbm] * 6,
        out_specs=vmem,
        scratch_shapes=[
            pltpu.VMEM((tok, width), BF16),
            slots, slots, slots, slots,
            pltpu.VMEM((many * SUB, LANES), F32),
            pltpu.VMEM((many, width), BF16),
            pltpu.VMEM((tok, width), F32),
            pltpu.VMEM((2, tok, LANES), jnp.int32),
            pltpu.VMEM((2, 8, tok), jnp.int32),
            pltpu.VMEM((2, width, half), BF16), pltpu.VMEM((2, width, half), BF16), pltpu.VMEM((2, half, width), BF16),
            pltpu.VMEM((2, width, half_shared), BF16), pltpu.VMEM((2, width, half_shared), BF16),
            pltpu.VMEM((2, half_shared, width), BF16),
            dma((6,)), dma((6,)), dma((6,)), dma, dma((NZ,)), dma, dma((NZ,)),
        ],
        compiler_params=pltpu.CompilerParams(
            collective_id=0, has_side_effects=True, vmem_limit_bytes=60 * 2**20
        ),
        name="moe",
    )(tokens, norm_gain.reshape(1, width), expert_ids, route_weights, eg, eu, ed, sg, su, sd)


def solution(mesh):
    placed = (
        P(("ep", "tp"), None),
        P(),
        P(("ep", "tp"), None),
        P(("ep", "tp"), None),
        P("ep", None, "tp"),
        P("ep", None, "tp"),
        P("ep", "tp", None),
        P(None, "tp"),
        P(None, "tp"),
        P("tp", None),
    )
    return jax.shard_map(
        body, mesh=mesh, in_specs=placed, out_specs=P(("ep", "tp"), None), check_vma=False
    )
```

```python
import jax
import jax.numpy as jnp
from jax import lax
from jax.experimental import pallas as pl
from jax.experimental.pallas import tpu as pltpu
from jax.sharding import PartitionSpec as P

MESH = pl.DeviceIdType.MESH
F32, BF16 = jnp.float32, jnp.bfloat16
epsilon = 1e-06
LANES, SUB = 128, 16
NZ, NY, NX = 8, 4, 4


def kernel(
    tokens_hbm, gain_ref, ids_ref, weights_ref, eg_ref, eu_ref, ed_ref, sg_ref, su_ref, sd_ref,
    out_ref,
    tokens_ref, normed, outgoing, received, results, returned, stage, rows, total, pcol, wcol, prow,
    wg, wu, wd, vg, vu, vd,
    token_sem, ready, local_sem, half_send, half_recv, out_send, out_recv, back_send, back_recv,
):
    plane = NY * NX
    experts = NZ * plane
    groups, group = plane // 2, 2 * NZ
    tok = tokens_ref.shape[0]
    capacity = received.shape[1] // SUB
    many = group * capacity
    me, core = lax.axis_index("ep"), lax.axis_index("tp")
    z, q = me // plane, me % plane
    place = q * NZ + z
    way = 1 - 2 * core

    load = pltpu.make_async_copy(tokens_hbm, tokens_ref, token_sem)
    load.start()

    def turn(step):
        odd = step % 2
        return odd * ((step + 1) // 2) + (1 - odd) * ((NZ - step // 2) % NZ)

    def ahead(step):
        return (z + way * turn(step) + NZ) % NZ

    def partner(step):
        pair, value, bit = q // 2, 0, 1
        while bit < groups:
            value = value + bit * ((pair // bit + step // bit) % 2)
            bit *= 2
        return value

    def member(step, i):
        there_q = 2 * partner(step) + (q + i // NZ) % 2
        there_z = ahead(i % NZ)
        return there_q * NZ + there_z, there_z * plane + there_q

    def first(step):
        return jnp.where(step == 0, 1, 0)

    barrier = pltpu.get_barrier_semaphore()

    def greet_along(i, carry):
        there = ahead(NZ - i) * plane + q
        pl.semaphore_signal(barrier, inc=1, device_id=(there, core), device_id_type=MESH)
        return carry

    def greet_across(semaphore):
        def greet(i, carry):
            there = z * plane + (q + i) % plane
            pl.semaphore_signal(semaphore, inc=1, device_id=(there, core), device_id_type=MESH)
            return carry

        lax.fori_loop(1, plane, greet, 0)

    lax.fori_loop(1, NZ, greet_along, 0)
    greet_across(barrier)
    pl.semaphore_signal(barrier, inc=1, device_id=(me, 1 - core), device_id_type=MESH)

    pairs = (
        (eg_ref.at[0], wg), (eu_ref.at[0], wu), (ed_ref.at[0], wd), (sg_ref, vg), (su_ref, vu), (sd_ref, vd),
    )
    own = [pltpu.make_async_copy(a, b.at[0], local_sem.at[i]) for i, (a, b) in enumerate(pairs)]
    other = [
        pltpu.make_async_remote_copy(
            src_ref=a, dst_ref=b.at[1], send_sem=half_send.at[i], recv_sem=half_recv.at[i],
            device_id=(me, 1 - core), device_id_type=MESH,
        )
        for i, (a, b) in enumerate(pairs)
    ]
    for copy in own:
        copy.start()

    expert_at = lax.broadcasted_iota(jnp.int32, (experts, tok), 0).astype(F32)
    earlier = (
        lax.broadcasted_iota(jnp.int32, (tok, tok), 0) < lax.broadcasted_iota(jnp.int32, (tok, tok), 1)
    ).astype(BF16)
    base = jnp.zeros((experts, 1), F32)
    for j in range(2):
        named = ids_ref[j : j + 1, :].astype(F32)
        high = jnp.floor(named * (1.0 / plane))
        named = (named - high * plane) * NZ + high
        hot = (named == expert_at).astype(F32)
        before = jnp.dot(hot.astype(BF16), earlier, preferred_element_type=F32) + base
        slot = jnp.sum(hot * before, axis=0, keepdims=True)
        base = base + jnp.sum(hot, axis=1, keepdims=True)
        prow[j : j + 1, :] = named * capacity + slot

    pl.semaphore_wait(barrier, NZ - 1 + plane - 1 + 1)
    greet_across(ready)
    load.wait()

    def from_block(block, c, width):
        for k in range(width // LANES):
            stage[pl.ds(c * (width // LANES) + k, many, stride=SUB), :] = block[:, k * LANES : (k + 1) * LANES]

    def to_flat(target, start):
        target[pl.ds(start, group)] = stage[...].astype(BF16).reshape(group, capacity * SUB, LANES)

    def from_flat(source, start):
        stage[...] = source[pl.ds(start, group)].reshape(many * SUB, LANES).astype(F32)

    def column(c):
        return stage[pl.ds(c, many, stride=SUB), :]

    def dispatch(step, carry):
        start = partner(step) * group
        slots = (lax.broadcasted_iota(jnp.int32, (many, tok), 0) + start * capacity).astype(F32)
        pick = ((slots == prow[0:1, :]) | (slots == prow[1:2, :])).astype(BF16)
        width = 256
        for c in range(SUB * LANES // width):
            from_block(
                jnp.dot(pick, tokens_ref[:, c * width : (c + 1) * width], preferred_element_type=F32), c, width
            )
        to_flat(outgoing, start)

        def send(i, carry):
            slot, there = member(step, i)
            pltpu.make_async_remote_copy(
                src_ref=outgoing.at[slot], dst_ref=received.at[place], send_sem=out_send,
                recv_sem=out_recv.at[step], device_id=(there, core), device_id_type=MESH,
            ).start()
            return carry

        @pl.when(step == 0)
        def _():
            pltpu.make_async_copy(outgoing.at[place], received.at[place], out_recv.at[0]).start()

        lax.fori_loop(first(step), NZ, send, 0)

        @pl.when(step == 0)
        def _():
            pl.semaphore_wait(ready, plane - 1)

        lax.fori_loop(NZ, group, send, 0)
        return carry

    lax.fori_loop(0, groups, dispatch, 0)
    for copy in other:
        copy.start()

    for j in range(2):
        pcol[j] = jnp.transpose(jnp.broadcast_to(prow[j : j + 1, :], (LANES, tok)))
        wcol[j] = jnp.transpose(jnp.broadcast_to(weights_ref[j : j + 1, :], (LANES, tok)))

    def gated(block, gate_w, up_w):
        parts = []
        for h in range(2):
            gate = jnp.dot(block, gate_w[h], preferred_element_type=F32)
            up = jnp.dot(block, up_w[h], preferred_element_type=F32)
            parts.append((gate / (1.0 + jnp.exp(-gate)) * up).astype(BF16))
        return parts

    def down(parts, down_w, c, width):
        return sum(
            jnp.dot(parts[h], down_w[h, :, c * width : (c + 1) * width], preferred_element_type=F32)
            for h in range(2)
        )

    for i in range(3):
        own[i].wait()
        other[i].wait()

    def expert(step, carry):
        start = partner(step) * group
        pltpu.make_async_remote_copy(
            src_ref=outgoing.at[pl.ds(0, group)], dst_ref=received.at[pl.ds(start, group)],
            send_sem=out_send, recv_sem=out_recv.at[step], device_id=(me, 1 - core), device_id_type=MESH,
        ).wait_recv()
        from_flat(received, start)
        squares = jnp.zeros((many, LANES), F32)
        for c in range(SUB):
            squares = squares + column(c) * column(c)
        mean = jnp.sum(squares, axis=1, keepdims=True) * (1.0 / (SUB * LANES))
        factor = lax.rsqrt(mean + epsilon)
        for c in range(SUB):
            lanes = slice(c * LANES, (c + 1) * LANES)
            rows[:, lanes] = (column(c) * factor * gain_ref[:, lanes]).astype(BF16)
        parts = gated(rows[...], wg, wu)
        for c in range(4):
            from_block(down(parts, wd, c, 512), c, 512)
        to_flat(results, start)

        def send(i, carry):
            slot, there = member(step, i)
            pltpu.make_async_remote_copy(
                src_ref=results.at[slot], dst_ref=returned.at[place], send_sem=back_send,
                recv_sem=back_recv.at[step], device_id=(there, core), device_id_type=MESH,
            ).start()
            return carry

        @pl.when(step == 0)
        def _():
            pltpu.make_async_copy(results.at[place], returned.at[place], back_recv.at[0]).start()

        lax.fori_loop(first(step), group, send, 0)
        return carry

    lax.fori_loop(0, groups, expert, 0)

    values = tokens_ref[...].astype(F32)
    scale = lax.rsqrt(jnp.mean(values * values, axis=1, keepdims=True) + epsilon)
    normed[...] = (values * scale * gain_ref[...]).astype(BF16)
    for i in range(3, 6):
        own[i].wait()
        other[i].wait()
    step_rows = tok // 2

    def shared(step, carry):
        at_rows = pl.ds(pl.multiple_of(step * step_rows, step_rows), step_rows)
        parts = gated(normed[at_rows, :], vg, vu)
        for c in range(4):
            total[at_rows, c * 512 : (c + 1) * 512] = down(parts, vd, c, 512)
        return carry

    lax.fori_loop(0, 2, shared, 0)

    def combine(step, carry):
        start = partner(step) * group
        slots = (lax.broadcasted_iota(jnp.int32, (tok, many), 1) + start * capacity).astype(F32)
        share = jnp.zeros((tok, many), F32)
        for j in range(2):
            share = share + jnp.where(slots == pcol[j, :, 0:1], wcol[j, :, 0:1], 0.0)
        high = share.astype(BF16)
        low = (share - high.astype(F32)).astype(BF16)
        pltpu.make_async_remote_copy(
            src_ref=results.at[pl.ds(0, group)], dst_ref=returned.at[pl.ds(start, group)],
            send_sem=back_send, recv_sem=back_recv.at[step], device_id=(me, 1 - core), device_id_type=MESH,
        ).wait_recv()
        from_flat(returned, start)
        for c in range(SUB):
            rows[:, c * LANES : (c + 1) * LANES] = column(c).astype(BF16)
        for c in range(4):
            part = rows[:, c * 512 : (c + 1) * 512]
            total[:, c * 512 : (c + 1) * 512] += jnp.dot(
                high, part, preferred_element_type=F32
            ) + jnp.dot(low, part, preferred_element_type=F32)
        return carry

    lax.fori_loop(0, groups, combine, 0)
    out_ref[...] = total[...].astype(BF16)

    pltpu.make_async_remote_copy(
        src_ref=outgoing.at[pl.ds(0, experts - 1)], dst_ref=received.at[pl.ds(0, experts - 1)],
        send_sem=out_send, recv_sem=out_recv.at[0], device_id=(me, 1 - core), device_id_type=MESH,
    ).wait_send()
    pltpu.make_async_remote_copy(
        src_ref=results.at[pl.ds(0, experts - 1)], dst_ref=returned.at[pl.ds(0, experts - 1)],
        send_sem=back_send, recv_sem=back_recv.at[0], device_id=(me, 1 - core), device_id_type=MESH,
    ).wait_send()


def body(tokens, norm_gain, expert_ids, route_weights, eg, eu, ed, sg, su, sd):
    tok, width = tokens.shape
    experts = eg.shape[0] * lax.axis_size("ep")
    capacity = 3 * tok * expert_ids.shape[1] // (2 * experts)
    many = 2 * NZ * capacity
    half, half_shared = eg.shape[2], sg.shape[1]
    slots = pltpu.VMEM((experts, capacity * SUB, LANES), BF16)
    vmem, hbm = pl.BlockSpec(memory_space=pltpu.VMEM), pl.BlockSpec(memory_space=pltpu.HBM)
    dma = pltpu.SemaphoreType.DMA

    def stay(array):
        return pltpu.with_memory_space_constraint(array, pltpu.HBM)

    return pl.pallas_call(
        kernel,
        out_shape=jax.ShapeDtypeStruct((tok, width), BF16),
        in_specs=[hbm] + [vmem] * 3 + [hbm] * 6,
        out_specs=vmem,
        scratch_shapes=[
            pltpu.VMEM((tok, width), BF16), pltpu.VMEM((tok, width), BF16),
            slots, slots, slots, slots,
            pltpu.VMEM((many * SUB, LANES), F32),
            pltpu.VMEM((many, width), BF16),
            pltpu.VMEM((tok, width), F32),
            pltpu.VMEM((2, tok, LANES), F32), pltpu.VMEM((2, tok, LANES), F32), pltpu.VMEM((8, tok), F32),
            pltpu.VMEM((2, width, half), BF16), pltpu.VMEM((2, width, half), BF16), pltpu.VMEM((2, half, width), BF16),
            pltpu.VMEM((2, width, half_shared), BF16), pltpu.VMEM((2, width, half_shared), BF16),
            pltpu.VMEM((2, half_shared, width), BF16),
            dma, pltpu.SemaphoreType.REGULAR, dma((6,)), dma((6,)), dma((6,)), dma, dma((NY * NX // 2,)), dma, dma((NY * NX // 2,)),
        ],
        compiler_params=pltpu.CompilerParams(
            collective_id=0, has_side_effects=True, vmem_limit_bytes=36 * 2**20
        ),
        name="moe",
    )(
        stay(tokens), stay(norm_gain.reshape(1, width)), stay(expert_ids.T), stay(route_weights.T),
        stay(eg), stay(eu), stay(ed), stay(sg), stay(su), stay(sd),
    )


def solution(mesh):
    placed = (
        P(("ep", "tp"), None),
        P(),
        P(("ep", "tp"), None),
        P(("ep", "tp"), None),
        P("ep", None, "tp"),
        P("ep", None, "tp"),
        P("ep", "tp", None),
        P(None, "tp"),
        P(None, "tp"),
        P("tp", None),
    )
    return jax.shard_map(
        body, mesh=mesh, in_specs=placed, out_specs=P(("ep", "tp"), None), check_vma=False
    )
```

```python
import jax
import jax.numpy as jnp
from jax import lax
from jax.experimental import pallas as pl
from jax.experimental.pallas import tpu as pltpu
from jax.sharding import PartitionSpec as P

MESH = pl.DeviceIdType.MESH
F32, BF16 = jnp.float32, jnp.bfloat16
epsilon = 1e-06
LANES, SUB = 128, 16
NZ, NY, NX = 8, 4, 4


def kernel(
    tokens_hbm, gain_ref, ids_ref, weights_ref, eg_ref, eu_ref, ed_ref, sg_ref, su_ref, sd_ref,
    out_ref,
    near, normed, outgoing, received, results, returned, stage, rows, total, pcol, wcol, slots_of,
    wg, wu, wd, vg, vu, vd,
    token_sem, ready, near_send, near_recv, local_sem, half_send, half_recv, out_send, out_recv, back_send, back_recv,
):
    group = NY * NX
    experts = NZ * group
    side = NZ // 2
    tok = near.shape[1]
    capacity = received.shape[1] // SUB
    many = group * capacity
    me, core = lax.axis_index("ep"), lax.axis_index("tp")
    z, y, x = me // group, (me // NX) % NY, me % NX
    q = me % group
    way = 1 - 2 * core

    load = pltpu.make_async_copy(tokens_hbm, near.at[0], token_sem)
    load.start()

    def along(distance):
        return (z + distance + NZ) % NZ

    def offset(step):
        return jnp.where(step > side, side - step, step)

    def across(i, sign):
        there_y = (y + sign * (i // NX) + NY) % NY
        there_x = (x + sign * (i % NX) + NX) % NX
        return there_y * NX + there_x

    def first(own):
        return jnp.where(own, 1, 0)

    barrier = pltpu.get_barrier_semaphore()

    def greet_along(i, carry):
        there = along(i) * group + q
        pl.semaphore_signal(barrier, inc=1, device_id=(there, core), device_id_type=MESH)
        return carry

    def greet_across(semaphore):
        def greet(i, carry):
            there = z * group + across(i, 1)
            pl.semaphore_signal(semaphore, inc=1, device_id=(there, core), device_id_type=MESH)
            return carry

        lax.fori_loop(1, group, greet, 0)

    lax.fori_loop(1, NZ, greet_along, 0)
    greet_across(barrier)
    pl.semaphore_signal(barrier, inc=1, device_id=(me, 1 - core), device_id_type=MESH)

    pairs = (
        (eg_ref.at[0], wg), (eu_ref.at[0], wu), (ed_ref.at[0], wd), (sg_ref, vg), (su_ref, vu), (sd_ref, vd),
    )
    own = [pltpu.make_async_copy(a, b.at[0], local_sem.at[i]) for i, (a, b) in enumerate(pairs)]
    other = [
        pltpu.make_async_remote_copy(
            src_ref=a, dst_ref=b.at[1], send_sem=half_send.at[i], recv_sem=half_recv.at[i],
            device_id=(me, 1 - core), device_id_type=MESH,
        )
        for i, (a, b) in enumerate(pairs)
    ]
    for copy in own:
        copy.start()

    expert_at = lax.broadcasted_iota(jnp.int32, (experts, tok), 0).astype(F32)
    earlier = (
        lax.broadcasted_iota(jnp.int32, (tok, tok), 0) < lax.broadcasted_iota(jnp.int32, (tok, tok), 1)
    ).astype(BF16)
    base = jnp.zeros((experts, 1), F32)
    for j in range(2):
        named = ids_ref[j : j + 1, :].astype(F32)
        hot = (named == expert_at).astype(F32)
        before = jnp.dot(hot.astype(BF16), earlier, preferred_element_type=F32) + base
        slot = jnp.sum(hot * before, axis=0, keepdims=True)
        base = base + jnp.sum(hot, axis=1, keepdims=True)
        slots_of[0, j : j + 1, :] = named * capacity + slot

    load.wait()
    pl.semaphore_wait(barrier, NZ - 1 + group - 1 + 1)

    def whole(path):
        there = along(way * (1 - 2 * path)) * group + q
        return [
            pltpu.make_async_remote_copy(
                src_ref=ref.at[0], dst_ref=ref.at[1 + path], send_sem=near_send.at[path, i],
                recv_sem=near_recv.at[path, i], device_id=(there, core), device_id_type=MESH,
            )
            for i, ref in enumerate((near, slots_of))
        ]

    ahead, behind = whole(0), whole(1)
    for copy in ahead:
        copy.start()
    greet_across(ready)

    def from_block(block, c, width):
        for k in range(width // LANES):
            stage[pl.ds(c * (width // LANES) + k, many, stride=SUB), :] = block[:, k * LANES : (k + 1) * LANES]

    def to_flat(target, start):
        target[pl.ds(start, group)] = stage[...].astype(BF16).reshape(group, capacity * SUB, LANES)

    def from_flat(source, start):
        stage[...] = source[pl.ds(start, group)].reshape(many * SUB, LANES).astype(F32)

    def column(c):
        return stage[pl.ds(c, many, stride=SUB), :]

    def dispatch(step, carry):
        path = (step + side - 1) // side
        hops = jnp.where(step == 0, 0, (step - 1) % side)
        sign = way * (3 - 2 * path) * first(step > 0)
        source = along(-sign) * group + q
        target = along(sign * hops)

        @pl.when(step == 1)
        def _():
            for copy in ahead:
                copy.wait_recv()

        @pl.when(step == side + 1)
        def _():
            for copy in behind:
                copy.wait_recv()

        wanted = (lax.broadcasted_iota(jnp.int32, (many, tok), 0) + target * many).astype(F32)
        pick = ((wanted == slots_of[path, 0:1, :]) | (wanted == slots_of[path, 1:2, :])).astype(BF16)
        width = 256
        for c in range(SUB * LANES // width):
            from_block(
                jnp.dot(pick, near[path, :, c * width : (c + 1) * width], preferred_element_type=F32), c, width
            )
        to_flat(outgoing, step * group)

        def send(i, carry):
            there = across(i, way)
            pltpu.make_async_remote_copy(
                src_ref=outgoing.at[step * group + there], dst_ref=received.at[source], send_sem=out_send,
                recv_sem=out_recv.at[step], device_id=(target * group + there, core), device_id_type=MESH,
            ).start()
            return carry

        @pl.when(hops == 0)
        def _():
            pltpu.make_async_copy(
                outgoing.at[step * group + q], received.at[source], out_recv.at[step]
            ).start()

        lax.fori_loop(first(hops == 0), group, send, 0)

        @pl.when(step == 0)
        def _():
            pl.semaphore_wait(ready, group - 1)
            for copy in ahead:
                copy.wait_send()
            for copy in behind:
                copy.start()

        return carry

    lax.fori_loop(0, NZ, dispatch, 0)
    for copy in other:
        copy.start()

    for j in range(2):
        pcol[j] = jnp.transpose(jnp.broadcast_to(slots_of[0, j : j + 1, :], (LANES, tok)))
        wcol[j] = jnp.transpose(jnp.broadcast_to(weights_ref[j : j + 1, :], (LANES, tok)))

    def gated(block, gate_w, up_w):
        parts = []
        for h in range(2):
            gate = jnp.dot(block, gate_w[h], preferred_element_type=F32)
            up = jnp.dot(block, up_w[h], preferred_element_type=F32)
            parts.append((gate / (1.0 + jnp.exp(-gate)) * up).astype(BF16))
        return parts

    def down(parts, down_w, c, width):
        return sum(
            jnp.dot(parts[h], down_w[h, :, c * width : (c + 1) * width], preferred_element_type=F32)
            for h in range(2)
        )

    for i in range(3):
        own[i].wait()
        other[i].wait()

    def expert(step, carry):
        start = along(-way * offset(step)) * group
        pltpu.make_async_remote_copy(
            src_ref=outgoing.at[pl.ds(0, group)], dst_ref=received.at[pl.ds(start, group)],
            send_sem=out_send, recv_sem=out_recv.at[step], device_id=(me, 1 - core), device_id_type=MESH,
        ).wait_recv()
        from_flat(received, start)
        squares = jnp.zeros((many, LANES), F32)
        for c in range(SUB):
            squares = squares + column(c) * column(c)
        mean = jnp.sum(squares, axis=1, keepdims=True) * (1.0 / (SUB * LANES))
        factor = lax.rsqrt(mean + epsilon)
        for c in range(SUB):
            lanes = slice(c * LANES, (c + 1) * LANES)
            rows[:, lanes] = (column(c) * factor * gain_ref[:, lanes]).astype(BF16)
        parts = gated(rows[...], wg, wu)
        for c in range(4):
            from_block(down(parts, wd, c, 512), c, 512)
        to_flat(results, start)

        def send(i, carry):
            there = start + across(i, -way)
            pltpu.make_async_remote_copy(
                src_ref=results.at[there], dst_ref=returned.at[me], send_sem=back_send,
                recv_sem=back_recv.at[step], device_id=(there, core), device_id_type=MESH,
            ).start()
            return carry

        @pl.when(step == 0)
        def _():
            pltpu.make_async_copy(results.at[me], returned.at[me], back_recv.at[0]).start()

        lax.fori_loop(first(step == 0), group, send, 0)
        return carry

    lax.fori_loop(0, NZ, expert, 0)

    values = near[0].astype(F32)
    scale = lax.rsqrt(jnp.mean(values * values, axis=1, keepdims=True) + epsilon)
    normed[...] = (values * scale * gain_ref[...]).astype(BF16)
    for i in range(3, 6):
        own[i].wait()
        other[i].wait()
    step_rows = tok // 2

    def shared(step, carry):
        at_rows = pl.ds(pl.multiple_of(step * step_rows, step_rows), step_rows)
        parts = gated(normed[at_rows, :], vg, vu)
        for c in range(4):
            total[at_rows, c * 512 : (c + 1) * 512] = down(parts, vd, c, 512)
        return carry

    lax.fori_loop(0, 2, shared, 0)

    def combine(step, carry):
        start = along(way * offset(step)) * group
        wanted = (lax.broadcasted_iota(jnp.int32, (tok, many), 1) + start * capacity).astype(F32)
        share = jnp.zeros((tok, many), F32)
        for j in range(2):
            share = share + jnp.where(wanted == pcol[j, :, 0:1], wcol[j, :, 0:1], 0.0)
        high = share.astype(BF16)
        low = (share - high.astype(F32)).astype(BF16)
        pltpu.make_async_remote_copy(
            src_ref=results.at[pl.ds(0, group)], dst_ref=returned.at[pl.ds(start, group)],
            send_sem=back_send, recv_sem=back_recv.at[step], device_id=(me, 1 - core), device_id_type=MESH,
        ).wait_recv()
        from_flat(returned, start)
        for c in range(SUB):
            rows[:, c * LANES : (c + 1) * LANES] = column(c).astype(BF16)
        for c in range(4):
            part = rows[:, c * 512 : (c + 1) * 512]
            total[:, c * 512 : (c + 1) * 512] += jnp.dot(
                high, part, preferred_element_type=F32
            ) + jnp.dot(low, part, preferred_element_type=F32)
        return carry

    lax.fori_loop(0, NZ, combine, 0)
    out_ref[...] = total[...].astype(BF16)

    for copy in behind:
        copy.wait_send()
    pltpu.make_async_remote_copy(
        src_ref=outgoing.at[pl.ds(0, experts - 3)], dst_ref=received.at[pl.ds(0, experts - 3)],
        send_sem=out_send, recv_sem=out_recv.at[0], device_id=(me, 1 - core), device_id_type=MESH,
    ).wait_send()
    pltpu.make_async_remote_copy(
        src_ref=results.at[pl.ds(0, experts - 1)], dst_ref=returned.at[pl.ds(0, experts - 1)],
        send_sem=back_send, recv_sem=back_recv.at[0], device_id=(me, 1 - core), device_id_type=MESH,
    ).wait_send()


def body(tokens, norm_gain, expert_ids, route_weights, eg, eu, ed, sg, su, sd):
    tok, width = tokens.shape
    experts = eg.shape[0] * lax.axis_size("ep")
    capacity = 3 * tok * expert_ids.shape[1] // (2 * experts)
    many = NY * NX * capacity
    half, half_shared = eg.shape[2], sg.shape[1]
    slots = pltpu.VMEM((experts, capacity * SUB, LANES), BF16)
    vmem, hbm = pl.BlockSpec(memory_space=pltpu.VMEM), pl.BlockSpec(memory_space=pltpu.HBM)
    dma = pltpu.SemaphoreType.DMA

    def stay(array):
        return pltpu.with_memory_space_constraint(array, pltpu.HBM)

    return pl.pallas_call(
        kernel,
        out_shape=jax.ShapeDtypeStruct((tok, width), BF16),
        in_specs=[hbm] + [vmem] * 3 + [hbm] * 6,
        out_specs=vmem,
        scratch_shapes=[
            pltpu.VMEM((3, tok, width), BF16), pltpu.VMEM((tok, width), BF16),
            slots, slots, slots, slots,
            pltpu.VMEM((many * SUB, LANES), F32),
            pltpu.VMEM((many, width), BF16),
            pltpu.VMEM((tok, width), F32),
            pltpu.VMEM((2, tok, LANES), F32), pltpu.VMEM((2, tok, LANES), F32), pltpu.VMEM((3, 8, tok), F32),
            pltpu.VMEM((2, width, half), BF16), pltpu.VMEM((2, width, half), BF16), pltpu.VMEM((2, half, width), BF16),
            pltpu.VMEM((2, width, half_shared), BF16), pltpu.VMEM((2, width, half_shared), BF16),
            pltpu.VMEM((2, half_shared, width), BF16),
            dma, pltpu.SemaphoreType.REGULAR, dma((2, 2)), dma((2, 2)), dma((6,)), dma((6,)), dma((6,)), dma, dma((NZ,)), dma, dma((NZ,)),
        ],
        compiler_params=pltpu.CompilerParams(
            collective_id=0, has_side_effects=True, vmem_limit_bytes=40 * 2**20
        ),
        name="moe",
    )(
        stay(tokens), stay(norm_gain.reshape(1, width)), stay(expert_ids.T), stay(route_weights.T),
        stay(eg), stay(eu), stay(ed), stay(sg), stay(su), stay(sd),
    )


def solution(mesh):
    placed = (
        P(("ep", "tp"), None),
        P(),
        P(("ep", "tp"), None),
        P(("ep", "tp"), None),
        P("ep", None, "tp"),
        P("ep", None, "tp"),
        P("ep", "tp", None),
        P(None, "tp"),
        P(None, "tp"),
        P("tp", None),
    )
    return jax.shard_map(
        body, mesh=mesh, in_specs=placed, out_specs=P(("ep", "tp"), None), check_vma=False
    )
```

```python
import jax
import jax.numpy as jnp
from jax import lax
from jax.experimental import pallas as pl
from jax.experimental.pallas import tpu as pltpu
from jax.sharding import PartitionSpec as P

MESH = pl.DeviceIdType.MESH
F32, BF16 = jnp.float32, jnp.bfloat16
epsilon = 1e-06
LANES, SUB = 128, 16
NZ, NY, NX = 8, 4, 4


def kernel(
    tokens_hbm, gain_ref, ids_ref, weights_ref, eg_ref, eu_ref, ed_ref, sg_ref, su_ref, sd_ref,
    out_ref,
    near, normed, outgoing, received, results, returned, stage, rows, total, pcol, wcol, slots_of,
    part_out, part_in,
    wg, wu, wd, vg, vu, vd,
    token_sem, ready, near_send, near_recv, part_send, part_recv, local_sem, half_send, half_recv, out_send, out_recv, back_send, back_recv,
):
    group = NY * NX
    experts = NZ * group
    side = NZ // 2
    tok = near.shape[1]
    capacity = received.shape[1] // SUB
    many = group * capacity
    me, core = lax.axis_index("ep"), lax.axis_index("tp")
    z, y, x = me // group, (me // NX) % NY, me % NX
    q = me % group
    way = 1 - 2 * core

    load = pltpu.make_async_copy(tokens_hbm, near.at[0], token_sem)
    load.start()

    def along(distance):
        return (z + distance + NZ) % NZ

    def offset(step):
        return jnp.where(step > side, side - step, step)

    def across(i, sign):
        there_y = (y + sign * (i // NX) + NY) % NY
        there_x = (x + sign * (i % NX) + NX) % NX
        return there_y * NX + there_x

    def first(own):
        return jnp.where(own, 1, 0)

    barrier = pltpu.get_barrier_semaphore()

    def greet_along(i, carry):
        there = along(i) * group + q
        pl.semaphore_signal(barrier, inc=1, device_id=(there, core), device_id_type=MESH)
        return carry

    def greet_across(semaphore):
        def greet(i, carry):
            there = z * group + across(i, 1)
            pl.semaphore_signal(semaphore, inc=1, device_id=(there, core), device_id_type=MESH)
            return carry

        lax.fori_loop(1, group, greet, 0)

    lax.fori_loop(1, NZ, greet_along, 0)
    greet_across(barrier)
    pl.semaphore_signal(barrier, inc=1, device_id=(me, 1 - core), device_id_type=MESH)

    pairs = (
        (eg_ref.at[0], wg), (eu_ref.at[0], wu), (ed_ref.at[0], wd), (sg_ref, vg), (su_ref, vu), (sd_ref, vd),
    )
    own = [pltpu.make_async_copy(a, b.at[0], local_sem.at[i]) for i, (a, b) in enumerate(pairs)]
    other = [
        pltpu.make_async_remote_copy(
            src_ref=a, dst_ref=b.at[1], send_sem=half_send.at[i], recv_sem=half_recv.at[i],
            device_id=(me, 1 - core), device_id_type=MESH,
        )
        for i, (a, b) in enumerate(pairs)
    ]
    for copy in own:
        copy.start()

    expert_at = lax.broadcasted_iota(jnp.int32, (experts, tok), 0).astype(F32)
    earlier = (
        lax.broadcasted_iota(jnp.int32, (tok, tok), 0) < lax.broadcasted_iota(jnp.int32, (tok, tok), 1)
    ).astype(BF16)
    base = jnp.zeros((experts, 1), F32)
    for j in range(2):
        named = ids_ref[j : j + 1, :].astype(F32)
        hot = (named == expert_at).astype(F32)
        before = jnp.dot(hot.astype(BF16), earlier, preferred_element_type=F32) + base
        slot = jnp.sum(hot * before, axis=0, keepdims=True)
        base = base + jnp.sum(hot, axis=1, keepdims=True)
        slots_of[0, j : j + 1, :] = named * capacity + slot
        slots_of[0, 2 + j : 3 + j, :] = weights_ref[j : j + 1, :]

    load.wait()
    pl.semaphore_wait(barrier, NZ - 1 + group - 1 + 1)

    def whole(path):
        there = along(way * (1 - 2 * path)) * group + q
        return [
            pltpu.make_async_remote_copy(
                src_ref=ref.at[0], dst_ref=ref.at[1 + path], send_sem=near_send.at[path, i],
                recv_sem=near_recv.at[path, i], device_id=(there, core), device_id_type=MESH,
            )
            for i, ref in enumerate((near, slots_of))
        ]

    ahead, behind = whole(0), whole(1)
    for copy in ahead:
        copy.start()
    greet_across(ready)

    def from_block(block, c, width):
        for k in range(width // LANES):
            stage[pl.ds(c * (width // LANES) + k, many, stride=SUB), :] = block[:, k * LANES : (k + 1) * LANES]

    def to_flat(target, start):
        target[pl.ds(start, group)] = stage[...].astype(BF16).reshape(group, capacity * SUB, LANES)

    def from_flat(source, start):
        stage[...] = source[pl.ds(start, group)].reshape(many * SUB, LANES).astype(F32)

    def column(c):
        return stage[pl.ds(c, many, stride=SUB), :]

    def route(step):
        path = (step + side - 1) // side
        hops = jnp.where(step == 0, 0, (step - 1) % side)
        return path, way * (3 - 2 * path) * first(step > 0), hops

    def dispatch(step, carry):
        path, sign, hops = route(step)
        source = along(-sign) * group + q
        target = along(sign * hops)

        @pl.when(step == 1)
        def _():
            for copy in ahead:
                copy.wait_recv()

        @pl.when(step == side + 1)
        def _():
            for copy in behind:
                copy.wait_recv()

        wanted = (lax.broadcasted_iota(jnp.int32, (many, tok), 0) + target * many).astype(F32)
        pick = ((wanted == slots_of[path, 0:1, :]) | (wanted == slots_of[path, 1:2, :])).astype(BF16)
        width = 256
        for c in range(SUB * LANES // width):
            from_block(
                jnp.dot(pick, near[path, :, c * width : (c + 1) * width], preferred_element_type=F32), c, width
            )
        to_flat(outgoing, step * group)

        def send(i, carry):
            there = across(i, way)
            pltpu.make_async_remote_copy(
                src_ref=outgoing.at[step * group + there], dst_ref=received.at[source], send_sem=out_send,
                recv_sem=out_recv.at[step], device_id=(target * group + there, core), device_id_type=MESH,
            ).start()
            return carry

        @pl.when(hops == 0)
        def _():
            pltpu.make_async_copy(
                outgoing.at[step * group + q], received.at[source], out_recv.at[step]
            ).start()

        lax.fori_loop(first(hops == 0), group, send, 0)

        @pl.when(step == 0)
        def _():
            pl.semaphore_wait(ready, group - 1)
            for copy in ahead:
                copy.wait_send()
            for copy in behind:
                copy.start()

        return carry

    lax.fori_loop(0, NZ, dispatch, 0)
    for copy in other:
        copy.start()

    for path in range(3):
        for j in range(2):
            for k, ref in ((0, pcol), (2, wcol)):
                row = slots_of[path, j + k : j + k + 1, :]
                ref[path, j] = jnp.transpose(jnp.broadcast_to(row, (LANES, tok)))

    def gated(block, gate_w, up_w):
        parts = []
        for h in range(2):
            gate = jnp.dot(block, gate_w[h], preferred_element_type=F32)
            up = jnp.dot(block, up_w[h], preferred_element_type=F32)
            parts.append((gate / (1.0 + jnp.exp(-gate)) * up).astype(BF16))
        return parts

    def down(parts, down_w, c, width):
        return sum(
            jnp.dot(parts[h], down_w[h, :, c * width : (c + 1) * width], preferred_element_type=F32)
            for h in range(2)
        )

    for i in range(3):
        own[i].wait()
        other[i].wait()

    def expert(step, carry):
        start = along(-way * offset(step)) * group
        pltpu.make_async_remote_copy(
            src_ref=outgoing.at[pl.ds(0, group)], dst_ref=received.at[pl.ds(start, group)],
            send_sem=out_send, recv_sem=out_recv.at[step], device_id=(me, 1 - core), device_id_type=MESH,
        ).wait_recv()
        from_flat(received, start)
        squares = jnp.zeros((many, LANES), F32)
        for c in range(SUB):
            squares = squares + column(c) * column(c)
        mean = jnp.sum(squares, axis=1, keepdims=True) * (1.0 / (SUB * LANES))
        factor = lax.rsqrt(mean + epsilon)
        for c in range(SUB):
            lanes = slice(c * LANES, (c + 1) * LANES)
            rows[:, lanes] = (column(c) * factor * gain_ref[:, lanes]).astype(BF16)
        parts = gated(rows[...], wg, wu)
        for c in range(4):
            from_block(down(parts, wd, c, 512), c, 512)
        to_flat(results, start)
        _, sign, hops = route(step)
        target = along(-sign * hops)

        def send(i, carry):
            there = across(i, -way)
            pltpu.make_async_remote_copy(
                src_ref=results.at[start + there], dst_ref=returned.at[step * group + q],
                send_sem=back_send, recv_sem=back_recv.at[step],
                device_id=(target * group + there, core), device_id_type=MESH,
            ).start()
            return carry

        @pl.when(hops == 0)
        def _():
            pltpu.make_async_copy(
                results.at[start + q], returned.at[step * group + q], back_recv.at[step]
            ).start()

        lax.fori_loop(first(hops == 0), group, send, 0)
        return carry

    lax.fori_loop(0, NZ, expert, 0)

    values = near[0].astype(F32)
    scale = lax.rsqrt(jnp.mean(values * values, axis=1, keepdims=True) + epsilon)
    normed[...] = (values * scale * gain_ref[...]).astype(BF16)
    for i in range(3, 6):
        own[i].wait()
        other[i].wait()
    step_rows = tok // 2

    def shared(step, carry):
        at_rows = pl.ds(pl.multiple_of(step * step_rows, step_rows), step_rows)
        parts = gated(normed[at_rows, :], vg, vu)
        for c in range(4):
            total[0, at_rows, c * 512 : (c + 1) * 512] = down(parts, vd, c, 512)
        return carry

    lax.fori_loop(0, 2, shared, 0)

    for path in range(1, 3):
        total[path] = jnp.zeros(total.shape[1:], F32)

    def summed(path):
        there = along(-way * (1 - 2 * path)) * group + q
        return pltpu.make_async_remote_copy(
            src_ref=part_out.at[path], dst_ref=part_in.at[path], send_sem=part_send.at[path],
            recv_sem=part_recv.at[path], device_id=(there, core), device_id_type=MESH,
        )

    def combine(turn, carry):
        step = (turn + 1) % NZ
        path, sign, hops = route(step)
        wanted = (
            lax.broadcasted_iota(jnp.int32, (tok, many), 1) + along(sign * hops) * many
        ).astype(F32)
        share = jnp.zeros((tok, many), F32)
        for j in range(2):
            share = share + jnp.where(wanted == pcol[path, j, :, 0:1], wcol[path, j, :, 0:1], 0.0)
        high = share.astype(BF16)
        low = (share - high.astype(F32)).astype(BF16)
        pltpu.make_async_remote_copy(
            src_ref=results.at[pl.ds(0, group)], dst_ref=returned.at[pl.ds(step * group, group)],
            send_sem=back_send, recv_sem=back_recv.at[step], device_id=(me, 1 - core), device_id_type=MESH,
        ).wait_recv()
        from_flat(returned, step * group)
        for c in range(SUB):
            rows[:, c * LANES : (c + 1) * LANES] = column(c).astype(BF16)
        for c in range(4):
            part = rows[:, c * 512 : (c + 1) * 512]
            total[path, :, c * 512 : (c + 1) * 512] += jnp.dot(
                high, part, preferred_element_type=F32
            ) + jnp.dot(low, part, preferred_element_type=F32)

        for path, last in ((0, side), (1, NZ - 1)):

            @pl.when(step == last)
            def _(path=path):
                part_out[path] = total[1 + path].astype(BF16)
                summed(path).start()

        return carry

    lax.fori_loop(0, NZ, combine, 0)
    for path in range(2):
        summed(path).wait_recv()
    out_ref[...] = (total[0] + (part_in[0].astype(F32) + part_in[1].astype(F32))).astype(BF16)

    for path in range(2):
        summed(path).wait_send()
    for copy in behind:
        copy.wait_send()
    pltpu.make_async_remote_copy(
        src_ref=outgoing.at[pl.ds(0, experts - 3)], dst_ref=received.at[pl.ds(0, experts - 3)],
        send_sem=out_send, recv_sem=out_recv.at[0], device_id=(me, 1 - core), device_id_type=MESH,
    ).wait_send()
    pltpu.make_async_remote_copy(
        src_ref=results.at[pl.ds(0, experts - 3)], dst_ref=returned.at[pl.ds(0, experts - 3)],
        send_sem=back_send, recv_sem=back_recv.at[0], device_id=(me, 1 - core), device_id_type=MESH,
    ).wait_send()


def body(tokens, norm_gain, expert_ids, route_weights, eg, eu, ed, sg, su, sd):
    tok, width = tokens.shape
    experts = eg.shape[0] * lax.axis_size("ep")
    capacity = 3 * tok * expert_ids.shape[1] // (2 * experts)
    many = NY * NX * capacity
    half, half_shared = eg.shape[2], sg.shape[1]
    slots = pltpu.VMEM((experts, capacity * SUB, LANES), BF16)
    vmem, hbm = pl.BlockSpec(memory_space=pltpu.VMEM), pl.BlockSpec(memory_space=pltpu.HBM)
    dma = pltpu.SemaphoreType.DMA

    def stay(array):
        return pltpu.with_memory_space_constraint(array, pltpu.HBM)

    return pl.pallas_call(
        kernel,
        out_shape=jax.ShapeDtypeStruct((tok, width), BF16),
        in_specs=[hbm] + [vmem] * 3 + [hbm] * 6,
        out_specs=vmem,
        scratch_shapes=[
            pltpu.VMEM((3, tok, width), BF16), pltpu.VMEM((tok, width), BF16),
            slots, slots, slots, slots,
            pltpu.VMEM((many * SUB, LANES), F32),
            pltpu.VMEM((many, width), BF16),
            pltpu.VMEM((3, tok, width), F32),
            pltpu.VMEM((3, 2, tok, LANES), F32), pltpu.VMEM((3, 2, tok, LANES), F32), pltpu.VMEM((3, 8, tok), F32),
            pltpu.VMEM((2, tok, width), BF16), pltpu.VMEM((2, tok, width), BF16),
            pltpu.VMEM((2, width, half), BF16), pltpu.VMEM((2, width, half), BF16), pltpu.VMEM((2, half, width), BF16),
            pltpu.VMEM((2, width, half_shared), BF16), pltpu.VMEM((2, width, half_shared), BF16),
            pltpu.VMEM((2, half_shared, width), BF16),
            dma, pltpu.SemaphoreType.REGULAR, dma((2, 2)), dma((2, 2)), dma((2,)), dma((2,)), dma((6,)), dma((6,)), dma((6,)), dma, dma((NZ,)), dma, dma((NZ,)),
        ],
        compiler_params=pltpu.CompilerParams(
            collective_id=0, has_side_effects=True, vmem_limit_bytes=50 * 2**20
        ),
        name="moe",
    )(
        stay(tokens), stay(norm_gain.reshape(1, width)), stay(expert_ids.T), stay(route_weights.T),
        stay(eg), stay(eu), stay(ed), stay(sg), stay(su), stay(sd),
    )


def solution(mesh):
    placed = (
        P(("ep", "tp"), None),
        P(),
        P(("ep", "tp"), None),
        P(("ep", "tp"), None),
        P("ep", None, "tp"),
        P("ep", None, "tp"),
        P("ep", "tp", None),
        P(None, "tp"),
        P(None, "tp"),
        P("tp", None),
    )
    return jax.shard_map(
        body, mesh=mesh, in_specs=placed, out_specs=P(("ep", "tp"), None), check_vma=False
    )
```

```python
import jax
import jax.numpy as jnp
from jax import lax
from jax.experimental import pallas as pl
from jax.experimental.pallas import tpu as pltpu
from jax.sharding import PartitionSpec as P

MESH = pl.DeviceIdType.MESH
F32, BF16 = jnp.float32, jnp.bfloat16
epsilon = 1e-06
LANES, SUB = 128, 16
NZ, NY, NX = 8, 4, 4


def kernel(
    tokens_hbm, gain_hbm, ids_hbm, weights_hbm, eg_ref, eu_ref, ed_ref, sg_ref, su_ref, sd_ref,
    out_ref,
    near, normed, outgoing, received, results, returned, stage, rows, twice, total, pcol, wcol, slots_of,
    part_out, part_in, gain_ref, ids_ref, weights_ref,
    wg, wu, wd, vg, vu, vd,
    token_sem, ready, near_send, near_recv, part_send, part_recv, small_sem, local_sem, half_send, half_recv, out_send, out_recv, back_send, back_recv,
):
    group = NY * NX
    experts = NZ * group
    side = NZ // 2
    tok = near.shape[1]
    capacity = received.shape[1] // SUB
    many = group * capacity
    me, core = lax.axis_index("ep"), lax.axis_index("tp")
    z, y, x = me // group, (me // NX) % NY, me % NX
    q = me % group
    way = 1 - 2 * core

    load = pltpu.make_async_copy(tokens_hbm, near.at[0], token_sem)
    small = [
        pltpu.make_async_copy(a, b, small_sem.at[i])
        for i, (a, b) in enumerate(((ids_hbm, ids_ref), (weights_hbm, weights_ref), (gain_hbm, gain_ref)))
    ]
    for copy in (*small, load):
        copy.start()

    def along(distance):
        return (z + distance + NZ) % NZ

    def offset(step):
        return jnp.where(step > side, side - step, step)

    def across(i, sign):
        there_y = (y + sign * (i // NX) + NY) % NY
        there_x = (x + sign * (i % NX) + NX) % NX
        return there_y * NX + there_x

    def first(own):
        return jnp.where(own, 1, 0)

    barrier = pltpu.get_barrier_semaphore()

    def greet_along(i, carry):
        there = along(i) * group + q
        pl.semaphore_signal(barrier, inc=1, device_id=(there, core), device_id_type=MESH)
        return carry

    def greet_across(semaphore):
        def greet(i, carry):
            there = z * group + across(i, 1)
            pl.semaphore_signal(semaphore, inc=1, device_id=(there, core), device_id_type=MESH)
            return carry

        lax.fori_loop(1, group, greet, 0)

    lax.fori_loop(1, NZ, greet_along, 0)
    greet_across(barrier)
    pl.semaphore_signal(barrier, inc=1, device_id=(me, 1 - core), device_id_type=MESH)

    pairs = (
        (eg_ref.at[0], wg), (eu_ref.at[0], wu), (ed_ref.at[0], wd), (sg_ref, vg), (su_ref, vu), (sd_ref, vd),
    )
    own = [pltpu.make_async_copy(a, b.at[0], local_sem.at[i]) for i, (a, b) in enumerate(pairs)]
    other = [
        pltpu.make_async_remote_copy(
            src_ref=a, dst_ref=b.at[1], send_sem=half_send.at[i], recv_sem=half_recv.at[i],
            device_id=(me, 1 - core), device_id_type=MESH,
        )
        for i, (a, b) in enumerate(pairs)
    ]
    for copy in own:
        copy.start()

    for copy in small:
        copy.wait()

    expert_at = lax.broadcasted_iota(jnp.int32, (experts, tok), 0).astype(F32)
    earlier = (
        lax.broadcasted_iota(jnp.int32, (tok, tok), 0) < lax.broadcasted_iota(jnp.int32, (tok, tok), 1)
    ).astype(BF16)
    base = jnp.zeros((experts, 1), F32)
    for j in range(2):
        named = ids_ref[j : j + 1, :].astype(F32)
        hot = (named == expert_at).astype(F32)
        before = jnp.dot(hot.astype(BF16), earlier, preferred_element_type=F32) + base
        slot = jnp.sum(hot * before, axis=0, keepdims=True)
        base = base + jnp.sum(hot, axis=1, keepdims=True)
        slots_of[0, j : j + 1, :] = named * capacity + slot
        slots_of[0, 2 + j : 3 + j, :] = weights_ref[j : j + 1, :]

    load.wait()
    pl.semaphore_wait(barrier, NZ - 1 + group - 1 + 1)

    def whole(path):
        there = along(way * (1 - 2 * path)) * group + q
        return [
            pltpu.make_async_remote_copy(
                src_ref=ref.at[0], dst_ref=ref.at[1 + path], send_sem=near_send.at[path, i],
                recv_sem=near_recv.at[path, i], device_id=(there, core), device_id_type=MESH,
            )
            for i, ref in enumerate((near, slots_of))
        ]

    ahead, behind = whole(0), whole(1)
    for copy in ahead:
        copy.start()
    greet_across(ready)

    def from_block(block, c, width):
        for k in range(width // LANES):
            stage[pl.ds(c * (width // LANES) + k, many, stride=SUB), :] = block[:, k * LANES : (k + 1) * LANES]

    def to_flat(target, start):
        target[pl.ds(start, group)] = stage[...].astype(BF16).reshape(group, capacity * SUB, LANES)

    def from_flat(source, start):
        stage[...] = source[pl.ds(start, group)].reshape(many * SUB, LANES).astype(F32)

    def column(c):
        return stage[pl.ds(c, many, stride=SUB), :]

    def route(step):
        path = (step + side - 1) // side
        hops = jnp.where(step == 0, 0, (step - 1) % side)
        return path, way * (3 - 2 * path) * first(step > 0), hops

    def dispatch(step, carry):
        path, sign, hops = route(step)
        source = along(-sign) * group + q
        target = along(sign * hops)

        @pl.when(step == 1)
        def _():
            for copy in ahead:
                copy.wait_recv()

        @pl.when(step == side + 1)
        def _():
            for copy in behind:
                copy.wait_recv()

        wanted = (lax.broadcasted_iota(jnp.int32, (many, tok), 0) + target * many).astype(F32)
        pick = ((wanted == slots_of[path, 0:1, :]) | (wanted == slots_of[path, 1:2, :])).astype(BF16)
        width = 256
        for c in range(SUB * LANES // width):
            from_block(
                jnp.dot(pick, near[path, :, c * width : (c + 1) * width], preferred_element_type=F32), c, width
            )
        to_flat(outgoing, step * group)

        def send(i, carry):
            there = across(i, way)
            pltpu.make_async_remote_copy(
                src_ref=outgoing.at[step * group + there], dst_ref=received.at[source], send_sem=out_send,
                recv_sem=out_recv.at[step], device_id=(target * group + there, core), device_id_type=MESH,
            ).start()
            return carry

        @pl.when(hops == 0)
        def _():
            pltpu.make_async_copy(
                outgoing.at[step * group + q], received.at[source], out_recv.at[step]
            ).start()

        lax.fori_loop(first(hops == 0), group, send, 0)

        @pl.when(step == 0)
        def _():
            pl.semaphore_wait(ready, group - 1)
            for copy in ahead:
                copy.wait_send()
            for copy in behind:
                copy.start()

        return carry

    lax.fori_loop(0, NZ, dispatch, 0)
    for copy in other:
        copy.start()

    for path in range(3):
        for j in range(2):
            for k, ref in ((0, pcol), (2, wcol)):
                row = slots_of[path, j + k : j + k + 1, :]
                ref[path, j] = jnp.transpose(jnp.broadcast_to(row, (LANES, tok)))

    def gated(block, gate_w, up_w):
        parts = []
        for h in range(2):
            gate = jnp.dot(block, gate_w[h], preferred_element_type=F32)
            up = jnp.dot(block, up_w[h], preferred_element_type=F32)
            parts.append((gate / (1.0 + jnp.exp(-gate)) * up).astype(BF16))
        return parts

    def down(parts, down_w, c, width):
        return sum(
            jnp.dot(parts[h], down_w[h, :, c * width : (c + 1) * width], preferred_element_type=F32)
            for h in range(2)
        )

    for i in range(3):
        own[i].wait()
        other[i].wait()

    def expert(step, carry):
        start = along(-way * offset(step)) * group
        pltpu.make_async_remote_copy(
            src_ref=outgoing.at[pl.ds(0, group)], dst_ref=received.at[pl.ds(start, group)],
            send_sem=out_send, recv_sem=out_recv.at[step], device_id=(me, 1 - core), device_id_type=MESH,
        ).wait_recv()
        from_flat(received, start)
        squares = jnp.zeros((many, LANES), F32)
        for c in range(SUB):
            squares = squares + column(c) * column(c)
        mean = jnp.sum(squares, axis=1, keepdims=True) * (1.0 / (SUB * LANES))
        factor = lax.rsqrt(mean + epsilon)
        for c in range(SUB):
            lanes = slice(c * LANES, (c + 1) * LANES)
            rows[:, lanes] = (column(c) * factor * gain_ref[:, lanes]).astype(BF16)
        parts = gated(rows[...], wg, wu)
        for c in range(4):
            from_block(down(parts, wd, c, 512), c, 512)
        to_flat(results, start)
        _, sign, hops = route(step)
        target = along(-sign * hops)

        def send(i, carry):
            there = across(i, -way)
            pltpu.make_async_remote_copy(
                src_ref=results.at[start + there], dst_ref=returned.at[step * group + q],
                send_sem=back_send, recv_sem=back_recv.at[step],
                device_id=(target * group + there, core), device_id_type=MESH,
            ).start()
            return carry

        @pl.when(hops == 0)
        def _():
            pltpu.make_async_copy(
                results.at[start + q], returned.at[step * group + q], back_recv.at[step]
            ).start()

        lax.fori_loop(first(hops == 0), group, send, 0)
        return carry

    lax.fori_loop(0, NZ, expert, 0)

    values = near[0].astype(F32)
    scale = lax.rsqrt(jnp.mean(values * values, axis=1, keepdims=True) + epsilon)
    normed[...] = (values * scale * gain_ref[...]).astype(BF16)
    for i in range(3, 6):
        own[i].wait()
        other[i].wait()
    step_rows = tok // 2

    def shared(step, carry):
        at_rows = pl.ds(pl.multiple_of(step * step_rows, step_rows), step_rows)
        parts = gated(normed[at_rows, :], vg, vu)
        for c in range(4):
            total[0, at_rows, c * 512 : (c + 1) * 512] = down(parts, vd, c, 512)
        return carry

    lax.fori_loop(0, 2, shared, 0)

    for path in range(1, 3):
        total[path] = jnp.zeros(total.shape[1:], F32)

    pieces = part_send.shape[1]
    piece = tok // pieces

    def summed(path, n):
        there = along(-way * (1 - 2 * path)) * group + q
        at_rows = pl.ds(n * piece, piece)
        return pltpu.make_async_remote_copy(
            src_ref=part_out.at[path, at_rows], dst_ref=part_in.at[path, at_rows],
            send_sem=part_send.at[path, n], recv_sem=part_recv.at[path, n],
            device_id=(there, core), device_id_type=MESH,
        )

    def combine(turn, carry):
        step = (turn + 1) % NZ
        path, sign, hops = route(step)
        wanted = (
            lax.broadcasted_iota(jnp.int32, (tok, many), 1) + along(sign * hops) * many
        ).astype(F32)
        share = jnp.zeros((tok, many), F32)
        for j in range(2):
            share = share + jnp.where(wanted == pcol[path, j, :, 0:1], wcol[path, j, :, 0:1], 0.0)
        high = share.astype(BF16)
        low = (share - high.astype(F32)).astype(BF16)
        both = jnp.concatenate([high, low], axis=1)
        pltpu.make_async_remote_copy(
            src_ref=results.at[pl.ds(0, group)], dst_ref=returned.at[pl.ds(step * group, group)],
            send_sem=back_send, recv_sem=back_recv.at[step], device_id=(me, 1 - core), device_id_type=MESH,
        ).wait_recv()
        from_flat(returned, step * group)
        for c in range(SUB):
            values = column(c).astype(BF16)
            twice[0:many, c * LANES : (c + 1) * LANES] = values
            twice[many:, c * LANES : (c + 1) * LANES] = values
        for c in range(4):
            total[path, :, c * 512 : (c + 1) * 512] += jnp.dot(
                both, twice[:, c * 512 : (c + 1) * 512], preferred_element_type=F32
            )

        for path, last in ((0, side), (1, NZ - 1)):

            @pl.when(step == last)
            def _(path=path):
                for n in range(pieces):
                    at_rows = pl.ds(n * piece, piece)
                    part_out[path, at_rows] = total[1 + path, at_rows].astype(BF16)
                    summed(path, n).start()

        return carry

    lax.fori_loop(0, NZ, combine, 0)
    for n in range(pieces):
        for path in range(2):
            summed(path, n).wait_recv()
        at_rows = pl.ds(n * piece, piece)
        added = part_in[0, at_rows].astype(F32) + part_in[1, at_rows].astype(F32)
        out_ref[at_rows, :] = (total[0, at_rows] + added).astype(BF16)

    for n in range(pieces):
        for path in range(2):
            summed(path, n).wait_send()
    for copy in behind:
        copy.wait_send()
    pltpu.make_async_remote_copy(
        src_ref=outgoing.at[pl.ds(0, experts - 3)], dst_ref=received.at[pl.ds(0, experts - 3)],
        send_sem=out_send, recv_sem=out_recv.at[0], device_id=(me, 1 - core), device_id_type=MESH,
    ).wait_send()
    pltpu.make_async_remote_copy(
        src_ref=results.at[pl.ds(0, experts - 3)], dst_ref=returned.at[pl.ds(0, experts - 3)],
        send_sem=back_send, recv_sem=back_recv.at[0], device_id=(me, 1 - core), device_id_type=MESH,
    ).wait_send()


def body(tokens, norm_gain, expert_ids, route_weights, eg, eu, ed, sg, su, sd):
    tok, width = tokens.shape
    experts = eg.shape[0] * lax.axis_size("ep")
    capacity = 3 * tok * expert_ids.shape[1] // (2 * experts)
    many = NY * NX * capacity
    half, half_shared = eg.shape[2], sg.shape[1]
    slots = pltpu.VMEM((experts, capacity * SUB, LANES), BF16)
    vmem, hbm = pl.BlockSpec(memory_space=pltpu.VMEM), pl.BlockSpec(memory_space=pltpu.HBM)
    dma = pltpu.SemaphoreType.DMA

    def stay(array):
        return pltpu.with_memory_space_constraint(array, pltpu.HBM)

    return pl.pallas_call(
        kernel,
        out_shape=jax.ShapeDtypeStruct((tok, width), BF16),
        in_specs=[hbm] * 10,
        out_specs=vmem,
        scratch_shapes=[
            pltpu.VMEM((3, tok, width), BF16), pltpu.VMEM((tok, width), BF16),
            slots, slots, slots, slots,
            pltpu.VMEM((many * SUB, LANES), F32),
            pltpu.VMEM((many, width), BF16), pltpu.VMEM((2 * many, width), BF16),
            pltpu.VMEM((3, tok, width), F32),
            pltpu.VMEM((3, 2, tok, LANES), F32), pltpu.VMEM((3, 2, tok, LANES), F32), pltpu.VMEM((3, 8, tok), F32),
            pltpu.VMEM((2, tok, width), BF16), pltpu.VMEM((2, tok, width), BF16),
            pltpu.VMEM((1, width), F32), pltpu.VMEM(expert_ids.T.shape, jnp.int32), pltpu.VMEM(route_weights.T.shape, F32),
            pltpu.VMEM((2, width, half), BF16), pltpu.VMEM((2, width, half), BF16), pltpu.VMEM((2, half, width), BF16),
            pltpu.VMEM((2, width, half_shared), BF16), pltpu.VMEM((2, width, half_shared), BF16),
            pltpu.VMEM((2, half_shared, width), BF16),
            dma, pltpu.SemaphoreType.REGULAR, dma((2, 2)), dma((2, 2)), dma((2, 4)), dma((2, 4)), dma((3,)), dma((6,)), dma((6,)), dma((6,)), dma, dma((NZ,)), dma, dma((NZ,)),
        ],
        compiler_params=pltpu.CompilerParams(
            collective_id=0, has_side_effects=True, vmem_limit_bytes=50 * 2**20
        ),
        name="moe",
    )(
        stay(tokens), stay(norm_gain.reshape(1, width)), stay(expert_ids.T), stay(route_weights.T),
        stay(eg), stay(eu), stay(ed), stay(sg), stay(su), stay(sd),
    )


def solution(mesh):
    placed = (
        P(("ep", "tp"), None),
        P(),
        P(("ep", "tp"), None),
        P(("ep", "tp"), None),
        P("ep", None, "tp"),
        P("ep", None, "tp"),
        P("ep", "tp", None),
        P(None, "tp"),
        P(None, "tp"),
        P("tp", None),
    )
    return jax.shard_map(
        body, mesh=mesh, in_specs=placed, out_specs=P(("ep", "tp"), None), check_vma=False
    )
```

```python
import jax
import jax.numpy as jnp
from jax import lax
from jax.experimental import pallas as pl
from jax.experimental.pallas import tpu as pltpu
from jax.sharding import PartitionSpec as P

MESH = pl.DeviceIdType.MESH
F32, BF16 = jnp.float32, jnp.bfloat16
epsilon = 1e-06
LANES, SUB = 128, 16
NZ, NY, NX = 8, 4, 4


def kernel(
    tokens_hbm, gain_hbm, ids_hbm, weights_hbm, eg_ref, eu_ref, ed_ref, sg_ref, su_ref, sd_ref,
    out_ref,
    near, normed, outgoing, received, results, returned, stage, rows, twice, total, pcol, wcol, slots_of,
    part_out, part_in, gain_ref, ids_ref, weights_ref,
    wg, wu, wd, vg, vu, vd,
    token_sem, ready, near_send, near_recv, part_send, part_recv, small_sem, local_sem, half_send, half_recv, out_send, out_recv, back_send, back_recv,
):
    group = NY * NX
    experts = NZ * group
    side = NZ // 2
    tok = near.shape[1]
    capacity = received.shape[1] // SUB
    many = group * capacity
    me, core = lax.axis_index("ep"), lax.axis_index("tp")
    z, y, x = me // group, (me // NX) % NY, me % NX
    q = me % group
    way = 1 - 2 * core

    load = pltpu.make_async_copy(tokens_hbm, near.at[0], token_sem)
    small = [
        pltpu.make_async_copy(a, b, small_sem.at[i])
        for i, (a, b) in enumerate(((ids_hbm, ids_ref), (weights_hbm, weights_ref), (gain_hbm, gain_ref)))
    ]
    for copy in (*small, load):
        copy.start()

    def along(distance):
        return (z + distance + NZ) % NZ

    def offset(step):
        return jnp.where(step > side, side - step, step)

    def across(i, sign):
        there_y = (y + sign * (i // NX) + NY) % NY
        there_x = (x + sign * (i % NX) + NX) % NX
        return there_y * NX + there_x

    def first(own):
        return jnp.where(own, 1, 0)

    barrier = pltpu.get_barrier_semaphore()

    def greet_along(i, carry):
        there = along(i) * group + q
        pl.semaphore_signal(barrier, inc=1, device_id=(there, core), device_id_type=MESH)
        return carry

    def greet_across(semaphore):
        def greet(i, carry):
            there = z * group + across(i, 1)
            pl.semaphore_signal(semaphore, inc=1, device_id=(there, core), device_id_type=MESH)
            return carry

        lax.fori_loop(1, group, greet, 0)

    lax.fori_loop(1, NZ, greet_along, 0)
    greet_across(barrier)
    pl.semaphore_signal(barrier, inc=1, device_id=(me, 1 - core), device_id_type=MESH)

    pairs = (
        (eg_ref.at[0], wg), (eu_ref.at[0], wu), (ed_ref.at[0], wd), (sg_ref, vg), (su_ref, vu), (sd_ref, vd),
    )
    own = [pltpu.make_async_copy(a, b.at[0], local_sem.at[i]) for i, (a, b) in enumerate(pairs)]
    other = [
        pltpu.make_async_remote_copy(
            src_ref=a, dst_ref=b.at[1], send_sem=half_send.at[i], recv_sem=half_recv.at[i],
            device_id=(me, 1 - core), device_id_type=MESH,
        )
        for i, (a, b) in enumerate(pairs)
    ]
    for copy in own:
        copy.start()

    load.wait()
    pl.semaphore_wait(barrier, NZ - 1 + group - 1 + 1)

    def whole(path):
        there = along(way * (1 - 2 * path)) * group + q
        return [
            pltpu.make_async_remote_copy(
                src_ref=ref.at[0], dst_ref=ref.at[1 + path], send_sem=near_send.at[path, i],
                recv_sem=near_recv.at[path, i], device_id=(there, core), device_id_type=MESH,
            )
            for i, ref in enumerate((near, slots_of))
        ]

    ahead, behind = whole(0), whole(1)
    ahead[0].start()
    greet_across(ready)

    for copy in small:
        copy.wait()

    expert_at = lax.broadcasted_iota(jnp.int32, (experts, tok), 0).astype(F32)
    earlier = (
        lax.broadcasted_iota(jnp.int32, (tok, tok), 0) < lax.broadcasted_iota(jnp.int32, (tok, tok), 1)
    ).astype(BF16)
    base = jnp.zeros((experts, 1), F32)
    for j in range(2):
        named = ids_ref[j : j + 1, :].astype(F32)
        hot = (named == expert_at).astype(F32)
        before = jnp.dot(hot.astype(BF16), earlier, preferred_element_type=F32) + base
        slot = jnp.sum(hot * before, axis=0, keepdims=True)
        base = base + jnp.sum(hot, axis=1, keepdims=True)
        slots_of[0, j : j + 1, :] = named * capacity + slot
        slots_of[0, 2 + j : 3 + j, :] = weights_ref[j : j + 1, :]
    ahead[1].start()

    def from_block(block, c, width):
        for k in range(width // LANES):
            stage[pl.ds(c * (width // LANES) + k, many, stride=SUB), :] = block[:, k * LANES : (k + 1) * LANES]

    def to_flat(target, start):
        target[pl.ds(start, group)] = stage[...].astype(BF16).reshape(group, capacity * SUB, LANES)

    def from_flat(source, start):
        stage[...] = source[pl.ds(start, group)].reshape(many * SUB, LANES).astype(F32)

    def column(c):
        return stage[pl.ds(c, many, stride=SUB), :]

    def route(step):
        path = (step + side - 1) // side
        hops = jnp.where(step == 0, 0, (step - 1) % side)
        return path, way * (3 - 2 * path) * first(step > 0), hops

    def dispatch(step, carry):
        path, sign, hops = route(step)
        source = along(-sign) * group + q
        target = along(sign * hops)

        @pl.when(step == 1)
        def _():
            for copy in ahead:
                copy.wait_recv()

        @pl.when(step == side + 1)
        def _():
            for copy in behind:
                copy.wait_recv()

        wanted = (lax.broadcasted_iota(jnp.int32, (many, tok), 0) + target * many).astype(F32)
        pick = ((wanted == slots_of[path, 0:1, :]) | (wanted == slots_of[path, 1:2, :])).astype(BF16)
        width = 256
        for c in range(SUB * LANES // width):
            from_block(
                jnp.dot(pick, near[path, :, c * width : (c + 1) * width], preferred_element_type=F32), c, width
            )
        to_flat(outgoing, step * group)

        def send(i, carry):
            there = across(i, way)
            pltpu.make_async_remote_copy(
                src_ref=outgoing.at[step * group + there], dst_ref=received.at[source], send_sem=out_send,
                recv_sem=out_recv.at[step], device_id=(target * group + there, core), device_id_type=MESH,
            ).start()
            return carry

        @pl.when(hops == 0)
        def _():
            pltpu.make_async_copy(
                outgoing.at[step * group + q], received.at[source], out_recv.at[step]
            ).start()

        lax.fori_loop(first(hops == 0), group, send, 0)

        @pl.when(step == 0)
        def _():
            pl.semaphore_wait(ready, group - 1)
            for copy in ahead:
                copy.wait_send()
            for copy in behind:
                copy.start()

        return carry

    lax.fori_loop(0, NZ, dispatch, 0)
    for copy in other:
        copy.start()

    for path in range(3):
        for j in range(2):
            for k, ref in ((0, pcol), (2, wcol)):
                row = slots_of[path, j + k : j + k + 1, :]
                ref[path, j] = jnp.transpose(jnp.broadcast_to(row, (LANES, tok)))

    def gated(block, gate_w, up_w):
        parts = []
        for h in range(2):
            gate = jnp.dot(block, gate_w[h], preferred_element_type=F32)
            up = jnp.dot(block, up_w[h], preferred_element_type=F32)
            parts.append((gate / (1.0 + jnp.exp(-gate)) * up).astype(BF16))
        return parts

    def down(parts, down_w, c, width):
        return sum(
            jnp.dot(parts[h], down_w[h, :, c * width : (c + 1) * width], preferred_element_type=F32)
            for h in range(2)
        )

    for i in range(3):
        own[i].wait()
        other[i].wait()

    def expert(step, carry):
        start = along(-way * offset(step)) * group
        pltpu.make_async_remote_copy(
            src_ref=outgoing.at[pl.ds(0, group)], dst_ref=received.at[pl.ds(start, group)],
            send_sem=out_send, recv_sem=out_recv.at[step], device_id=(me, 1 - core), device_id_type=MESH,
        ).wait_recv()
        from_flat(received, start)
        squares = jnp.zeros((many, LANES), F32)
        for c in range(SUB):
            squares = squares + column(c) * column(c)
        mean = jnp.sum(squares, axis=1, keepdims=True) * (1.0 / (SUB * LANES))
        factor = lax.rsqrt(mean + epsilon)
        for c in range(SUB):
            lanes = slice(c * LANES, (c + 1) * LANES)
            rows[:, lanes] = (column(c) * factor * gain_ref[:, lanes]).astype(BF16)
        parts = gated(rows[...], wg, wu)
        for c in range(4):
            from_block(down(parts, wd, c, 512), c, 512)
        to_flat(results, start)
        _, sign, hops = route(step)
        target = along(-sign * hops)

        def send(i, carry):
            there = across(i, -way)
            pltpu.make_async_remote_copy(
                src_ref=results.at[start + there], dst_ref=returned.at[step * group + q],
                send_sem=back_send, recv_sem=back_recv.at[step],
                device_id=(target * group + there, core), device_id_type=MESH,
            ).start()
            return carry

        @pl.when(hops == 0)
        def _():
            pltpu.make_async_copy(
                results.at[start + q], returned.at[step * group + q], back_recv.at[step]
            ).start()

        lax.fori_loop(first(hops == 0), group, send, 0)
        return carry

    lax.fori_loop(0, NZ, expert, 0)

    values = near[0].astype(F32)
    scale = lax.rsqrt(jnp.mean(values * values, axis=1, keepdims=True) + epsilon)
    normed[...] = (values * scale * gain_ref[...]).astype(BF16)
    for i in range(3, 6):
        own[i].wait()
        other[i].wait()
    step_rows = tok // 2

    def shared(step, carry):
        at_rows = pl.ds(pl.multiple_of(step * step_rows, step_rows), step_rows)
        parts = gated(normed[at_rows, :], vg, vu)
        for c in range(4):
            total[0, at_rows, c * 512 : (c + 1) * 512] = down(parts, vd, c, 512)
        return carry

    lax.fori_loop(0, 2, shared, 0)

    for path in range(1, 3):
        total[path] = jnp.zeros(total.shape[1:], F32)

    pieces = part_send.shape[1]
    piece = tok // pieces

    def summed(path, n):
        there = along(-way * (1 - 2 * path)) * group + q
        at_rows = pl.ds(n * piece, piece)
        return pltpu.make_async_remote_copy(
            src_ref=part_out.at[path, at_rows], dst_ref=part_in.at[path, at_rows],
            send_sem=part_send.at[path, n], recv_sem=part_recv.at[path, n],
            device_id=(there, core), device_id_type=MESH,
        )

    def combine(turn, carry):
        step = (turn + 1) % NZ
        path, sign, hops = route(step)
        wanted = (
            lax.broadcasted_iota(jnp.int32, (tok, many), 1) + along(sign * hops) * many
        ).astype(F32)
        share = jnp.zeros((tok, many), F32)
        for j in range(2):
            share = share + jnp.where(wanted == pcol[path, j, :, 0:1], wcol[path, j, :, 0:1], 0.0)
        high = share.astype(BF16)
        low = (share - high.astype(F32)).astype(BF16)
        both = jnp.concatenate([high, low], axis=1)
        pltpu.make_async_remote_copy(
            src_ref=results.at[pl.ds(0, group)], dst_ref=returned.at[pl.ds(step * group, group)],
            send_sem=back_send, recv_sem=back_recv.at[step], device_id=(me, 1 - core), device_id_type=MESH,
        ).wait_recv()
        from_flat(returned, step * group)
        for c in range(SUB):
            values = column(c).astype(BF16)
            twice[0:many, c * LANES : (c + 1) * LANES] = values
            twice[many:, c * LANES : (c + 1) * LANES] = values
        for c in range(4):
            total[path, :, c * 512 : (c + 1) * 512] += jnp.dot(
                both, twice[:, c * 512 : (c + 1) * 512], preferred_element_type=F32
            )

        for path, last in ((0, side), (1, NZ - 1)):

            @pl.when(step == last)
            def _(path=path):
                for n in range(pieces):
                    at_rows = pl.ds(n * piece, piece)
                    part_out[path, at_rows] = total[1 + path, at_rows].astype(BF16)
                    summed(path, n).start()

        return carry

    lax.fori_loop(0, NZ, combine, 0)
    for n in range(pieces):
        for path in range(2):
            summed(path, n).wait_recv()
        at_rows = pl.ds(n * piece, piece)
        added = part_in[0, at_rows].astype(F32) + part_in[1, at_rows].astype(F32)
        out_ref[at_rows, :] = (total[0, at_rows] + added).astype(BF16)

    for n in range(pieces):
        for path in range(2):
            summed(path, n).wait_send()
    for copy in behind:
        copy.wait_send()
    pltpu.make_async_remote_copy(
        src_ref=outgoing.at[pl.ds(0, experts - 3)], dst_ref=received.at[pl.ds(0, experts - 3)],
        send_sem=out_send, recv_sem=out_recv.at[0], device_id=(me, 1 - core), device_id_type=MESH,
    ).wait_send()
    pltpu.make_async_remote_copy(
        src_ref=results.at[pl.ds(0, experts - 3)], dst_ref=returned.at[pl.ds(0, experts - 3)],
        send_sem=back_send, recv_sem=back_recv.at[0], device_id=(me, 1 - core), device_id_type=MESH,
    ).wait_send()


def body(tokens, norm_gain, expert_ids, route_weights, eg, eu, ed, sg, su, sd):
    tok, width = tokens.shape
    experts = eg.shape[0] * lax.axis_size("ep")
    capacity = 3 * tok * expert_ids.shape[1] // (2 * experts)
    many = NY * NX * capacity
    half, half_shared = eg.shape[2], sg.shape[1]
    slots = pltpu.VMEM((experts, capacity * SUB, LANES), BF16)
    vmem, hbm = pl.BlockSpec(memory_space=pltpu.VMEM), pl.BlockSpec(memory_space=pltpu.HBM)
    dma = pltpu.SemaphoreType.DMA

    def stay(array):
        return pltpu.with_memory_space_constraint(array, pltpu.HBM)

    return pl.pallas_call(
        kernel,
        out_shape=jax.ShapeDtypeStruct((tok, width), BF16),
        in_specs=[hbm] * 10,
        out_specs=vmem,
        scratch_shapes=[
            pltpu.VMEM((3, tok, width), BF16), pltpu.VMEM((tok, width), BF16),
            slots, slots, slots, slots,
            pltpu.VMEM((many * SUB, LANES), F32),
            pltpu.VMEM((many, width), BF16), pltpu.VMEM((2 * many, width), BF16),
            pltpu.VMEM((3, tok, width), F32),
            pltpu.VMEM((3, 2, tok, LANES), F32), pltpu.VMEM((3, 2, tok, LANES), F32), pltpu.VMEM((3, 8, tok), F32),
            pltpu.VMEM((2, tok, width), BF16), pltpu.VMEM((2, tok, width), BF16),
            pltpu.VMEM((1, width), F32), pltpu.VMEM(expert_ids.T.shape, jnp.int32), pltpu.VMEM(route_weights.T.shape, F32),
            pltpu.VMEM((2, width, half), BF16), pltpu.VMEM((2, width, half), BF16), pltpu.VMEM((2, half, width), BF16),
            pltpu.VMEM((2, width, half_shared), BF16), pltpu.VMEM((2, width, half_shared), BF16),
            pltpu.VMEM((2, half_shared, width), BF16),
            dma, pltpu.SemaphoreType.REGULAR, dma((2, 2)), dma((2, 2)), dma((2, 4)), dma((2, 4)), dma((3,)), dma((6,)), dma((6,)), dma((6,)), dma, dma((NZ,)), dma, dma((NZ,)),
        ],
        compiler_params=pltpu.CompilerParams(
            collective_id=0, has_side_effects=True, vmem_limit_bytes=50 * 2**20
        ),
        name="moe",
    )(
        stay(tokens), stay(norm_gain.reshape(1, width)), stay(expert_ids.T), stay(route_weights.T),
        stay(eg), stay(eu), stay(ed), stay(sg), stay(su), stay(sd),
    )


def solution(mesh):
    placed = (
        P(("ep", "tp"), None),
        P(),
        P(("ep", "tp"), None),
        P(("ep", "tp"), None),
        P("ep", None, "tp"),
        P("ep", None, "tp"),
        P("ep", "tp", None),
        P(None, "tp"),
        P(None, "tp"),
        P("tp", None),
    )
    return jax.shard_map(
        body, mesh=mesh, in_specs=placed, out_specs=P(("ep", "tp"), None), check_vma=False
    )
```
